32 devices in a mesh: sp: 4 (over z), tp: 8 (over y, x, core).
Axes of the slice: x: 2, y: 2, z: 4, core: 2. Of those that a mesh axis runs over, the one named last changes fastest.
Arguments:
- latent: bfloat16 [1024, 4096], P(('sp', 'tp')), may hold values from -16 to 16
- context: bfloat16 [256, 4096], P('sp'), may hold values from -16 to 16
- cond: bfloat16 [4096], P('sp'), may hold values from -6 to 6
- cond_ctx: bfloat16 [4096], P('sp'), may hold values from -6 to 6
- mod_shift_w: bfloat16 [4096, 4096], P('sp', 'tp'), may hold values from -0.15625 to 0.15625
- mod_scale_w: bfloat16 [4096, 4096], P('sp', 'tp'), may hold values from -0.15625 to 0.15625
- mod_gate_w: bfloat16 [4096, 4096], P('sp', 'tp'), may hold values from -0.15625 to 0.15625
- norm_gain: bfloat16 [4096], replicated, may hold values from 0.099609375 to 1.8984375
- proj_z: bfloat16 [4096, 4096], P(None, 'tp'), may hold values from -0.09375 to 0.09375
- proj_x: bfloat16 [4096, 4096], P(None, 'tp'), may hold values from -0.09375 to 0.09375
- proj_b: bfloat16 [4096, 8192], P(None, 'tp'), may hold values from -0.09375 to 0.09375
- proj_c: bfloat16 [4096, 8192], P(None, 'tp'), may hold values from -0.09375 to 0.09375
- proj_dt: bfloat16 [4096, 128], replicated, may hold values from -0.09375 to 0.09375
- conv_x: bfloat16 [3, 4096], P(None, 'tp'), may hold values from -3.5 to 3.5
- conv_b: bfloat16 [3, 8192], P(None, 'tp'), may hold values from -3.5 to 3.5
- conv_c: bfloat16 [3, 8192], P(None, 'tp'), may hold values from -3.5 to 3.5
- dt_bias: float32 [128], P('tp'), may hold values from -1 to 1
- decay_log: float32 [128], P('tp'), may hold values from -11.6 to -2.9
- head_gain: bfloat16 [4096], P('tp'), may hold values from 0.099609375 to 1.8984375
- proj_out: bfloat16 [4096, 4096], P(None, 'tp'), may hold values from -0.09375 to 0.09375
Outputs:
- mixed: bfloat16 [1024, 4096], P(('sp', 'tp'))
The draws below stay inside these ranges and needn't reach their ends.
All inputs are finite; a program needn't handle non-finite values.
Results may differ from the reference program's by a relative error of at most 0.0065.
Values may be sent and summed in bfloat16 or wider, within the bound.
No kernel may reach another device: no remote copies, remote signals or barrier semaphores. Data moves between devices by JAX's collectives and lax.ppermute only.
A program may use at most 128 MiB of HBM per device.

```python
import jax
import jax.numpy as jnp
from jax import lax

D = 4096
HEADS = 64
HEAD_DIM = 64
STATE = 128
BLOCK = 128
CTX = 256
SEQ = 1024


def draw_latent(key, part):
    key_noise = jax.random.fold_in(key, 11)
    key_dir = jax.random.fold_in(key, 12)
    key_level = jax.random.fold_in(key, 13)
    direction = jax.random.normal(key_dir, (D,), jnp.float32)
    levels = jax.random.uniform(key_level, (SEQ // BLOCK,), jnp.float32, -1.5, 1.5)
    offsets = jnp.repeat(levels, BLOCK, total_repeat_length=SEQ)[:, None] * direction[None, :]
    noise = jax.random.normal(key_noise, (SEQ, D), jnp.float32)
    return jnp.clip(noise + offsets, -16.0, 16.0).astype(jnp.bfloat16)


def draw_context(key, part):
    key_noise = jax.random.fold_in(key, 31)
    key_seg = jax.random.fold_in(key, 32)
    segment = CTX // 16
    directions = jax.random.normal(key_seg, (16, D), jnp.float32) * 4.0
    offsets = jnp.repeat(directions, segment, axis=0, total_repeat_length=CTX)
    noise = jax.random.normal(key_noise, (CTX, D), jnp.float32) * 0.7
    return jnp.clip(noise + offsets, -16.0, 16.0).astype(jnp.bfloat16)


def draw_decay_log(key, part):
    key_pick = jax.random.fold_in(key, 21)
    key_slow = jax.random.fold_in(key, 22)
    key_fast = jax.random.fold_in(key, 23)
    slow = jax.random.uniform(key_slow, (2 * HEADS,), jnp.float32, -11.5, -9.45)
    fast = jax.random.uniform(key_fast, (2 * HEADS,), jnp.float32, -4.2, -3.0)
    share = 0.5
    pick = jax.random.uniform(key_pick, (2 * HEADS,), jnp.float32) < share
    return jnp.where(pick, fast, slow)


def shard_levels(key, dims, shards, least, largest):
    level, own = 1.0, jax.random.fold_in(key, 6)
    for axis_at, blocks in shards:
        draws = jnp.exp(jax.random.uniform(jax.random.fold_in(own, axis_at), (blocks,), jnp.float32, least / len(shards), largest / len(shards)))
        level = level * jnp.repeat(draws, dims[axis_at] // blocks).reshape([-1 if axis == axis_at else 1 for axis in range(len(dims))])
    return level


def scatter_about(rng, shape, deviation, most, split=(), dtype=jnp.bfloat16):
    loudness = shard_levels(rng, shape, split, -0.22, 0.18) if split else 1.0
    array = jax.random.normal(rng, shape, jnp.float32) * deviation * loudness
    return jnp.minimum(jnp.maximum(array, -most), most).astype(dtype)


def setup_inputs(seed: int = 0) -> dict:
    keys = jax.random.split(jax.random.key(seed), 21)
    latent = draw_latent(jax.random.fold_in(keys[20], 71), 0)
    context = draw_context(jax.random.fold_in(keys[20], 71), 0)
    cond = scatter_about(keys[2], (D,), 1.0, 6.0, ((0, 4),))
    cond_ctx = scatter_about(keys[3], (D,), 1.0, 6.0, ((0, 4),))
    mod_shift_w = scatter_about(keys[4], (D, D), (D // 3) ** -0.5, 0.15625, ((0, 4), (1, 8)))
    mod_scale_w = scatter_about(keys[5], (D, D), (D // 3) ** -0.5, 0.15625, ((0, 4), (1, 8)))
    mod_gate_w = scatter_about(keys[6], (D, D), (D // 3) ** -0.5, 0.15625, ((0, 4), (1, 8)))
    norm_gain = jnp.clip(1.0 + 0.18 * jax.random.normal(keys[7], (D,), jnp.float32), 0.099609375, 1.8984375).astype(jnp.bfloat16)
    proj_z = scatter_about(keys[8], (D, D), D ** -0.5, 0.09375, ((1, 8),))
    proj_x = scatter_about(keys[9], (D, D), D ** -0.5, 0.09375, ((1, 8),))
    proj_b = scatter_about(keys[10], (D, HEADS * STATE), D ** -0.5, 0.09375, ((1, 8),))
    proj_c = scatter_about(keys[11], (D, HEADS * STATE), D ** -0.5, 0.09375, ((1, 8),))
    proj_dt = scatter_about(keys[12], (D, 2 * HEADS), D ** -0.5, 0.09375)
    conv_x = scatter_about(keys[13], (3, D), 3 ** -0.5, 3.5, ((1, 8),))
    conv_b = scatter_about(keys[14], (3, HEADS * STATE), 3 ** -0.5, 3.5, ((1, 8),))
    conv_c = scatter_about(keys[15], (3, HEADS * STATE), 3 ** -0.5, 3.5, ((1, 8),))
    dt_bias = jnp.clip(jax.random.uniform(keys[16], (2 * HEADS,), jnp.float32, -1.0, 1.0) * shard_levels(keys[16], (2 * HEADS,), ((0, 8),), -0.4, 0.0), -1.0, 1.0)
    decay_log = draw_decay_log(jax.random.fold_in(keys[20], 71), 0)
    head_gain = jnp.clip(1.0 + 0.18 * jax.random.normal(keys[18], (D,), jnp.float32), 0.099609375, 1.8984375).astype(jnp.bfloat16)
    proj_out = scatter_about(keys[19], (D, D), D ** -0.5, 0.09375, ((1, 8),))
    return dict(latent=latent, context=context, cond=cond, cond_ctx=cond_ctx, mod_shift_w=mod_shift_w, mod_scale_w=mod_scale_w, mod_gate_w=mod_gate_w, norm_gain=norm_gain, proj_z=proj_z, proj_x=proj_x, proj_b=proj_b, proj_c=proj_c, proj_dt=proj_dt, conv_x=conv_x, conv_b=conv_b, conv_c=conv_c, dt_bias=dt_bias, decay_log=decay_log, head_gain=head_gain, proj_out=proj_out)


EPS = 1e-06

def modulated_norm(rows, gain, shift, scale):
    wide = rows.astype(jnp.float32)
    normed = wide * lax.rsqrt(lax.optimization_barrier(jnp.mean(wide * wide, axis=-1, keepdims=True)) + EPS) * gain.astype(jnp.float32)
    return (normed * (1.0 + scale) + shift).astype(jnp.bfloat16)

def project(rows, weights):
    outputs = [jnp.dot(rows, w, preferred_element_type=jnp.float32).astype(jnp.bfloat16) for w in weights]
    return lax.optimization_barrier(outputs)

def centred_conv(padded, taps):
    wide = padded.astype(jnp.float32)
    weights = taps.astype(jnp.float32)
    length = padded.shape[0] - 2
    return jax.nn.silu(weights[0] * wide[:length] + weights[1] * wide[1:length + 1] + weights[2] * wide[2:])

def zero_pad(values):
    return jnp.pad(values, ((1, 1), (0, 0)))

def block_states(values, writes, step_size, decay_rate, block):
    length, heads, width = values.shape
    state = writes.shape[2]
    count = length // block
    log_decay = jnp.cumsum(-(step_size * decay_rate).reshape(count, block, heads), axis=1)
    scaled_values = (values * step_size[:, :, None]).reshape(count, block, heads, width)
    write_blocks = writes.reshape(count, block, heads, state)
    tail = jnp.exp(log_decay[:, -1:] - log_decay)
    block_sums = jnp.einsum('kshn,ksh,kshp->khpn', write_blocks, tail, scaled_values, precision=lax.Precision.HIGHEST)
    block_decay = jnp.exp(log_decay[:, -1])

    def advance(carry, inputs):
        block_sum, decay = inputs
        return (carry * decay[:, None, None] + block_sum, carry)
    final, entering = lax.scan(advance, jnp.zeros((heads, width, state), jnp.float32), (block_sums, block_decay))
    overall = jnp.exp(lax.optimization_barrier(jnp.sum(log_decay[:, -1], axis=0)))
    return (log_decay, scaled_values, entering, final, overall)

def block_outputs(reads, writes, log_decay, scaled_values, entering, start_state):
    count, block, heads = log_decay.shape
    state = reads.shape[2]
    read_blocks = reads.reshape(count, block, heads, state)
    write_blocks = writes.reshape(count, block, heads, state)
    starts = jnp.cumsum(log_decay[:, -1], axis=0) - log_decay[:, -1]
    entering_all = entering + jnp.exp(starts)[:, :, None, None] * start_state[None]
    forward_mask = jnp.tril(jnp.ones((block, block), bool))[None, :, :, None]
    spans = log_decay[:, :, None, :] - log_decay[:, None, :, :]
    weights = jnp.where(forward_mask, jnp.exp(jnp.where(forward_mask, spans, 0.0)), 0.0)
    intersection = jnp.einsum('kqhn,kshn->kqsh', read_blocks, write_blocks, precision=lax.Precision.HIGHEST)
    within = jnp.einsum('kqsh,kshp->kqhp', intersection * weights, scaled_values, precision=lax.Precision.HIGHEST)
    carried = jnp.einsum('kqhn,khpn->kqhp', read_blocks, entering_all, precision=lax.Precision.HIGHEST) * jnp.exp(log_decay)[..., None]
    return (within + carried).reshape(count * block, heads, -1)

def reference(latent, context, cond, cond_ctx, mod_shift_w, mod_scale_w, mod_gate_w, norm_gain, proj_z, proj_x, proj_b, proj_c, proj_dt, conv_x, conv_b, conv_c, dt_bias, decay_log, head_gain, proj_out):
    act = jax.nn.silu(cond.astype(jnp.float32)).astype(jnp.bfloat16)
    act_ctx = jax.nn.silu(cond_ctx.astype(jnp.float32)).astype(jnp.bfloat16)
    shift = jnp.dot(act, mod_shift_w, preferred_element_type=jnp.float32)
    scale = jnp.dot(act, mod_scale_w, preferred_element_type=jnp.float32)
    gate = jnp.dot(act, mod_gate_w, preferred_element_type=jnp.float32)
    ctx_shift = jnp.dot(act_ctx, mod_shift_w, preferred_element_type=jnp.float32)
    ctx_scale = jnp.dot(act_ctx, mod_scale_w, preferred_element_type=jnp.float32)
    normed_rows = modulated_norm(latent, norm_gain, shift, scale)
    normed_ctx = modulated_norm(context, norm_gain, ctx_shift, ctx_scale)
    x_in, b_in, c_in, z_in, dt_raw = project(normed_rows, (proj_x, proj_b, proj_c, proj_z, proj_dt))
    x_ctx, b_ctx, dt_ctx = project(normed_ctx, (proj_x, proj_b, proj_dt))
    values = centred_conv(zero_pad(x_in), conv_x).reshape(SEQ, HEADS, HEAD_DIM)
    writes = centred_conv(zero_pad(b_in), conv_b).reshape(SEQ, HEADS, STATE)
    reads = centred_conv(zero_pad(c_in), conv_c).reshape(SEQ, HEADS, STATE)
    values_ctx = centred_conv(zero_pad(x_ctx), conv_x).reshape(CTX, HEADS, HEAD_DIM)
    writes_ctx = centred_conv(zero_pad(b_ctx), conv_b).reshape(CTX, HEADS, STATE)
    step_size = jax.nn.softplus(dt_raw.astype(jnp.float32) + dt_bias).reshape(SEQ, HEADS, 2)
    step_ctx = jax.nn.softplus(dt_ctx.astype(jnp.float32) + dt_bias).reshape(CTX, HEADS, 2)
    decay_rate = jnp.exp(decay_log).reshape(HEADS, 2)
    ctx_f = block_states(values_ctx, writes_ctx, step_ctx[:, :, 0], decay_rate[:, 0], BLOCK)[3]
    ctx_b = block_states(jnp.flip(values_ctx, 0), jnp.flip(writes_ctx, 0), jnp.flip(step_ctx[:, :, 1], 0), decay_rate[:, 1], BLOCK)[3]
    log_f, scaled_f, enter_f, _, _ = block_states(values, writes, step_size[:, :, 0], decay_rate[:, 0], BLOCK)
    out_f = block_outputs(reads, writes, log_f, scaled_f, enter_f, ctx_f)
    log_b, scaled_b, enter_b, _, _ = block_states(jnp.flip(values, 0), jnp.flip(writes, 0), jnp.flip(step_size[:, :, 1], 0), decay_rate[:, 1], BLOCK)
    out_b = block_outputs(jnp.flip(reads, 0), jnp.flip(writes, 0), log_b, scaled_b, enter_b, ctx_b)
    summed = out_f + jnp.flip(out_b, 0)
    gated = summed * jax.nn.silu(z_in.astype(jnp.float32)).reshape(SEQ, HEADS, HEAD_DIM)
    gated = gated * lax.rsqrt(lax.optimization_barrier(jnp.mean(gated * gated, axis=-1, keepdims=True)) + EPS)
    gated = gated * head_gain.astype(jnp.float32).reshape(HEADS, HEAD_DIM)
    mixed_heads = gated.reshape(SEQ, D).astype(jnp.bfloat16)
    update = jnp.dot(mixed_heads, proj_out, preferred_element_type=jnp.float32).astype(jnp.bfloat16)
    update = lax.optimization_barrier(update).astype(jnp.float32)
    return (latent.astype(jnp.float32) + gate * update).astype(jnp.bfloat16)
```

```python
import functools

import jax
import jax.numpy as jnp
from jax import lax
from jax.experimental import pallas as pl
from jax.experimental.pallas import tpu as pltpu
from jax.sharding import PartitionSpec as P

HEAD_DIM = 64
LANES = 128
EPS = 1e-06
F32 = jnp.float32
BF16 = jnp.bfloat16
VMEM = pl.BlockSpec(memory_space=pltpu.VMEM)
HBM = pl.BlockSpec(memory_space=pltpu.HBM)
LIMIT = 56 * 1024 * 1024


def silu(u):
    return u * (0.5 * jnp.tanh(0.5 * u) + 0.5)


def call(kernel, outs, inputs, specs, scratch=(), flops=0, moved=0, name=None):
    return pl.pallas_call(
        kernel,
        out_shape=outs,
        in_specs=specs,
        out_specs=jax.tree.map(lambda _: VMEM, outs),
        scratch_shapes=list(scratch),
        compiler_params=pltpu.CompilerParams(vmem_limit_bytes=LIMIT),
        cost_estimate=pl.CostEstimate(flops=flops, bytes_accessed=moved, transcendentals=0),
        name=name,
    )(*inputs)


def shift(array, axis, step):
    count = lax.axis_size(axis)
    return lax.ppermute(array, axis, [(i, (i + step) % count) for i in range(count)])


def swap(array, bits):
    count = lax.axis_size("tp")
    return lax.ppermute(array, "tp", [(i, i ^ bits) for i in range(count)])


def direct(tp_count):
    return tp_count <= 8 and tp_count & (tp_count - 1) == 0 and tp_count > 1


def exchange_tp(array, dim):
    count = lax.axis_size("tp")
    if not direct(count):
        return [lax.all_gather(array, "tp", axis=dim, tiled=True)]
    pieces = [array, None] + [None] * (count - 2)
    for q in range(2, count, 2):
        pieces[q] = swap(array, q)
    for q in range(0, count, 2):
        pieces[q + 1] = swap(pieces[q], 1)
    return pieces


def mod_kernel(cond, cond_ctx, rows, w_shift, w_scale, w_gate, up, down):
    width = w_shift.shape[1]
    act = silu(cond[...].astype(F32)).astype(BF16)
    act_ctx = silu(cond_ctx[...].astype(F32)).astype(BF16)
    both = jnp.concatenate([act, act_ctx], axis=0)
    parts = [jnp.dot(both, w[...], preferred_element_type=F32) for w in (w_shift, w_scale, w_gate)]
    mods = jnp.concatenate(parts + [jnp.zeros((2, width), F32)], axis=0)
    pieces = rows.shape[1] // width
    first = rows[0:1, :].astype(F32)
    last = rows[rows.shape[0] - 1 :, :].astype(F32)
    for out, row in ((up, last), (down, first)):
        out[0:8, :] = mods
        for r in range(pieces):
            out[8 + r : 9 + r, :] = row[:, r * width : (r + 1) * width]


def mod_parts(cond, cond_ctx, latent, w_shift, w_scale, w_gate):
    width = w_shift.shape[1]
    shape = jax.ShapeDtypeStruct((8 + latent.shape[1] // width, width), F32)
    return call(
        mod_kernel,
        [shape, shape],
        [cond[None], cond_ctx[None], latent, w_shift, w_scale, w_gate],
        [VMEM] * 6,
        flops=12 * w_shift.size,
        moved=6 * w_shift.size,
        name="mod_parts",
    )


def assemble_kernel(*refs):
    pieces, mods, halo = refs[:-2], refs[-2], refs[-1]
    tp = lax.axis_index("tp")
    count = len(pieces)
    width = pieces[0].shape[1]
    halo[...] = jnp.zeros_like(halo)
    for q, piece in enumerate(pieces):
        source = tp ^ q
        mods[:, pl.ds(pl.multiple_of(source * width, width), width)] = piece[0:8, :]
        for at, owner in ((0, count - 1), (1, 0)):

            @pl.when(source == owner)
            def _(at=at, piece=piece):
                for r in range(count):
                    halo[at : at + 1, r * width : (r + 1) * width] = piece[8 + r : 9 + r, :]


def assemble(pieces, tp_count):
    if direct(tp_count):
        width = pieces[0].shape[1] * tp_count
        return call(
            assemble_kernel,
            [jax.ShapeDtypeStruct((8, width), F32), jax.ShapeDtypeStruct((8, width), F32)],
            pieces,
            [VMEM] * len(pieces),
            name="assemble",
        )
    (whole,) = pieces
    width = whole.shape[1]
    part = width // tp_count
    before = whole[8:, width - part :].reshape(1, width)
    after = whole[8:, :part].reshape(1, width)
    return whole[:8], jnp.concatenate([before, after, jnp.zeros((6, width), F32)])


def modulate(rows, gain, shift_row):
    wide = rows.astype(F32)
    return wide * lax.rsqrt(jnp.mean(wide * wide, axis=-1, keepdims=True) + EPS) * gain + shift_row


def conv_block(value, length, taps, before, after):
    centre = value[:length]
    row = lax.broadcasted_iota(jnp.int32, centre.shape, 0)
    earlier = jnp.where(row == 0, before, pltpu.roll(centre, 1, 0))
    later = jnp.where(row == length - 1, after, pltpu.roll(centre, length - 1, 0))
    return silu(taps[0:1] * earlier + taps[1:2] * centre + taps[2:3] * later)


def column_blocks(widths):
    blocks = []
    for which, width in enumerate(widths):
        step = min(width, 256)
        blocks += [(which, at, step) for at in range(0, width, step)]
    return blocks


def rounded(value):
    return value.astype(BF16).astype(F32)


def recurrence_kernel(places, length, heads, latent, sp_count, *refs):
    refs = list(refs)
    pieces = [refs.pop(0) for _ in places]
    mods = refs.pop(0)
    halo = refs.pop(0) if latent else None
    gain, bias, decay_log, w_dt, taps_x, taps_b, w_x, w_b = refs[:8]
    refs = refs[8:]
    if latent:
        h, xs, bs, cum_out, cum_t_out, step_t_out = refs[:6]
        messages = refs[6 : 6 + sp_count - 1]
        buffers = refs[6 + sp_count - 1 :]
    else:
        states_out, h, xs, bs = refs[:4]
        buffers = refs[4:]
    *slots, sems = buffers
    blocks = column_blocks((w_x.shape[1], w_b.shape[1]))
    copies = []
    for i, (which, at, width) in enumerate(blocks):
        source = (w_x, w_b)[which].at[:, at : at + width]
        copies.append(pltpu.make_async_copy(source, slots[i], sems.at[i]))
        copies[-1].start()
    sp = lax.axis_index("sp")
    tp = lax.axis_index("tp")
    kind = 0 if latent else 1
    shift_row = mods[kind : kind + 1, :]
    gain_row = gain[...].astype(F32) * (1.0 + mods[2 + kind : 3 + kind, :])
    for piece, (place, size, group) in zip(pieces, places):
        for at in range(0, piece.shape[0], 16):
            size_now = min(16, piece.shape[0] - at)
            offset = place(sp, tp, at)
            if not isinstance(offset, int):
                offset = pl.multiple_of(offset, 16)
            h[pl.ds(offset, size_now), :] = modulate(
                piece[at : at + size_now, :], gain_row, shift_row
            ).astype(BF16)
    if latent:
        edge = modulate(halo[...], gain_row, shift_row)
        pad = jnp.zeros((h.shape[0] - length - 8, edge.shape[1]), F32)
        h[length:, :] = jnp.concatenate([edge, pad], axis=0).astype(BF16)
    dt = rounded(jnp.dot(h[...], w_dt[...], preferred_element_type=F32))[:length]
    turn = lax.rem(LANES - tp * (2 * heads), LANES)
    dt = pltpu.roll(dt, turn, 1)
    biased = dt + bias[...]
    step = jnp.maximum(biased, 0.0) + jnp.log1p(jnp.exp(-jnp.abs(biased)))
    spent = step * jnp.exp(decay_log[...])
    row = lax.broadcasted_iota(jnp.int32, (length, length), 0)
    col = lax.broadcasted_iota(jnp.int32, (length, length), 1)
    lower = jnp.where(row >= col, 1.0, 0.0).astype(F32)
    upper = jnp.where(row <= col, 1.0, 0.0).astype(F32)
    high = lax.Precision.HIGHEST
    prefix = jnp.dot(lower, spent, precision=high, preferred_element_type=F32)
    suffix = jnp.dot(upper, spent, precision=high, preferred_element_type=F32)
    lane = lax.broadcasted_iota(jnp.int32, (length, LANES), 1)
    cum = -jnp.where(lane % 2 == 0, prefix, suffix)
    total = jnp.where(lane[0:1] % 2 == 0, cum[length - 1 : length], cum[0:1])
    weight = jnp.exp(total - cum) * step
    if latent:
        cum_t = cum.T
        cum_out[...] = cum
        cum_t_out[...] = cum_t
        step_t_out[...] = step.T
        extra = messages[0].shape[0] - heads * HEAD_DIM
        rows = extra // 2
        ends = cum_t[0:rows]
        parity = lax.broadcasted_iota(jnp.int32, (rows, 1), 0) % 2
        ends = jnp.where(parity == 0, ends[:, length - 1 : length], ends[:, 0:1])
        decay = jnp.broadcast_to(jnp.exp(ends), (rows, LANES))
        decay_hi = decay.astype(BF16)
        decay_lo = (decay - decay_hi.astype(F32)).astype(BF16)
        for message in messages:
            message[heads * HEAD_DIM : heads * HEAD_DIM + rows, :] = decay_hi
            message[heads * HEAD_DIM + rows :, :] = decay_lo
        has_before = jnp.where(sp > 0, 1.0, 0.0)
        has_after = jnp.where(sp < sp_count - 1, 1.0, 0.0)
    for i, (which, at, width) in enumerate(blocks):
        copies[i].wait()
        value = rounded(jnp.dot(h[...], slots[i][...], preferred_element_type=F32))
        taps = (taps_x, taps_b)[which][:, at : at + width].astype(F32)
        if latent:
            before = value[length : length + 1] * has_before
            after = value[length + 1 : length + 2] * has_after
        else:
            before = after = 0.0
        out = conv_block(value, length, taps, before, after)
        (xs, bs)[which][:, at : at + width] = out.astype(BF16)
    state = w_b.shape[1] // heads
    for head in range(heads):
        mine = xs[:, head * HEAD_DIM : (head + 1) * HEAD_DIM].astype(F32)
        pair = jnp.concatenate(
            [mine * weight[:, 2 * head : 2 * head + 1], mine * weight[:, 2 * head + 1 : 2 * head + 2]],
            axis=1,
        ).astype(BF16)
        states = lax.dot_general(
            pair,
            bs[:, head * state : (head + 1) * state],
            (((0,), (0,)), ((), ())),
            preferred_element_type=F32,
        )
        if latent:
            for k, message in enumerate(messages, 1):
                forward = sp + k < sp_count
                chosen = jnp.where(forward, states[:HEAD_DIM], states[HEAD_DIM:])
                message[head * HEAD_DIM : (head + 1) * HEAD_DIM, :] = chosen.astype(BF16)
        else:
            states_out[head * 2 * HEAD_DIM : (head + 1) * 2 * HEAD_DIM, :] = states


def padded_row(values):
    return jnp.pad(values, (0, LANES - values.shape[0]))[None]


def recurrence(places, pieces, length, heads, latent, mods, halo, common, sp_count, name):
    gain, bias, decay_log, w_dt, taps_x, taps_b, w_x, w_b = common
    depth = w_x.shape[0]
    state = w_b.shape[1] // heads
    struct = jax.ShapeDtypeStruct
    rows = length + 16 if latent else length
    if latent:
        extra = 2 * max(16, -(-2 * heads // 16) * 16)
        message = struct((heads * HEAD_DIM + extra, state), BF16)
        outs = [
            struct((rows, depth), BF16),
            struct((length, heads * HEAD_DIM), BF16),
            struct((length, heads * state), BF16),
            struct((length, LANES), F32),
            struct((LANES, length), F32),
            struct((LANES, length), F32),
        ] + [message] * (sp_count - 1)
        scratch = []
    else:
        outs = [struct((heads * 2 * HEAD_DIM, state), F32)]
        scratch = [
            pltpu.VMEM((rows, depth), BF16),
            pltpu.VMEM((length, heads * HEAD_DIM), BF16),
            pltpu.VMEM((length, heads * state), BF16),
        ]
    blocks = column_blocks((w_x.shape[1], w_b.shape[1]))
    scratch += [pltpu.VMEM((depth, width), BF16) for _, _, width in blocks]
    scratch += [pltpu.SemaphoreType.DMA((len(blocks),))]
    inputs = list(pieces) + [mods] + ([halo] if latent else []) + list(common)
    specs = [VMEM] * (len(inputs) - 2) + [HBM] * 2
    columns = w_x.shape[1] + w_b.shape[1]
    return call(
        functools.partial(recurrence_kernel, places, length, heads, latent, sp_count),
        outs,
        inputs,
        specs,
        scratch,
        flops=2 * rows * depth * columns,
        moved=2 * depth * columns,
        name=name,
    )


def outputs_kernel(length, heads, sp_count, *refs):
    h, xs, bs, cum, cum_t, step_t, taps_c, w_c, w_z, cs, y, zs, *buffers = refs
    *slots, sems = buffers
    blocks = column_blocks((w_c.shape[1], w_z.shape[1]))
    copies = []
    for i, (which, at, width) in enumerate(blocks):
        source = (w_c, w_z)[which].at[:, at : at + width]
        copies.append(pltpu.make_async_copy(source, slots[i], sems.at[i]))
        copies[-1].start()
    sp = lax.axis_index("sp")
    has_before = jnp.where(sp > 0, 1.0, 0.0)
    has_after = jnp.where(sp < sp_count - 1, 1.0, 0.0)
    for i, (which, at, width) in enumerate(blocks):
        copies[i].wait()
        value = rounded(jnp.dot(h[...], slots[i][...], preferred_element_type=F32))
        if which == 0:
            before = value[length : length + 1] * has_before
            after = value[length + 1 : length + 2] * has_after
            taps = taps_c[:, at : at + width].astype(F32)
            cs[:, at : at + width] = conv_block(value, length, taps, before, after).astype(BF16)
        else:
            zs[:, at : at + width] = silu(value[:length])
    state = w_c.shape[1] // heads
    row = lax.broadcasted_iota(jnp.int32, (length, length), 0)
    col = lax.broadcasted_iota(jnp.int32, (length, length), 1)
    for head in range(heads):
        f, b = 2 * head, 2 * head + 1
        meet = lax.dot_general(
            cs[:, head * state : (head + 1) * state],
            bs[:, head * state : (head + 1) * state],
            (((1,), (1,)), ((), ())),
            preferred_element_type=F32,
        )
        span = jnp.where(
            row >= col,
            cum[:, f : f + 1] - cum_t[f : f + 1, :],
            cum[:, b : b + 1] - cum_t[b : b + 1, :],
        )
        ahead, behind = step_t[f : f + 1, :], step_t[b : b + 1, :]
        steps = jnp.where(row > col, ahead, jnp.where(row < col, behind, ahead + behind))
        mixed = (meet * jnp.exp(span) * steps).astype(BF16)
        y[:, head * HEAD_DIM : (head + 1) * HEAD_DIM] = jnp.dot(
            mixed, xs[:, head * HEAD_DIM : (head + 1) * HEAD_DIM], preferred_element_type=F32
        )


def block_outputs(heads, length, sp_count, h, xs, bs, cum, cum_t, step_t, taps_c, w_c, w_z):
    struct = jax.ShapeDtypeStruct
    depth = w_c.shape[0]
    blocks = column_blocks((w_c.shape[1], w_z.shape[1]))
    columns = w_c.shape[1] + w_z.shape[1]
    return call(
        functools.partial(outputs_kernel, length, heads, sp_count),
        [
            struct((length, w_c.shape[1]), BF16),
            struct((length, w_z.shape[1]), F32),
            struct((length, w_z.shape[1]), F32),
        ],
        [h, xs, bs, cum, cum_t, step_t, taps_c, w_c, w_z],
        [VMEM] * 7 + [HBM] * 2,
        [pltpu.VMEM((depth, width), BF16) for _, _, width in blocks]
        + [pltpu.SemaphoreType.DMA((len(blocks),))],
        flops=2 * h.shape[0] * depth * columns,
        moved=2 * depth * columns,
        name="block_outputs",
    )


def finish_kernel(heads, sp_count, *refs):
    messages = refs[: sp_count - 1]
    ctx, cs, y, zs, cum, gain, out = refs[sp_count - 1 :]
    sp = lax.axis_index("sp")
    base = heads * HEAD_DIM
    rows = (messages[0].shape[0] - base) // 2
    decays = [
        m[base : base + rows, :].astype(F32) + m[base + rows :, :].astype(F32) for m in messages
    ]
    one = jnp.ones_like(decays[0])
    zero = jnp.zeros_like(decays[0])
    forward, backward = [None] * (sp_count - 1), [None] * (sp_count - 1)
    run = one
    for k in range(1, sp_count):
        active = k <= sp
        forward[k - 1] = jnp.where(active, run, zero)
        run = jnp.where(active, run * decays[k - 1], run)
    ctx_forward = run
    run = one
    for k in range(sp_count - 1, 0, -1):
        active = k > sp
        backward[k - 1] = jnp.where(active, run, zero)
        run = jnp.where(active, run * decays[k - 1], run)
    ctx_backward = run
    carry = jnp.exp(cum[...])
    state = cs.shape[1] // heads
    for head in range(heads):
        f, b = 2 * head, 2 * head + 1
        at = head * 2 * HEAD_DIM
        start_f = ctx[at : at + HEAD_DIM, :] * ctx_forward[f : f + 1]
        start_b = ctx[at + HEAD_DIM : at + 2 * HEAD_DIM, :] * ctx_backward[b : b + 1]
        for k in range(sp_count - 1):
            part = messages[k][head * HEAD_DIM : (head + 1) * HEAD_DIM, :].astype(F32)
            start_f = start_f + part * forward[k][f : f + 1]
            start_b = start_b + part * backward[k][b : b + 1]
        start = jnp.concatenate([start_f, start_b], axis=0).astype(BF16)
        carried = lax.dot_general(
            cs[:, head * state : (head + 1) * state],
            start,
            (((1,), (1,)), ((), ())),
            preferred_element_type=F32,
        )
        cols = slice(head * HEAD_DIM, (head + 1) * HEAD_DIM)
        total = (
            y[:, cols]
            + carried[:, :HEAD_DIM] * carry[:, f : f + 1]
            + carried[:, HEAD_DIM:] * carry[:, b : b + 1]
        )
        gated = total * zs[:, cols]
        scale = lax.rsqrt(jnp.mean(gated * gated, axis=-1, keepdims=True) + EPS)
        out[:, cols] = (gated * scale * gain[:, cols].astype(F32)).astype(BF16)


def finish(heads, sp_count, messages, ctx, cs, y, zs, cum, gain):
    inputs = list(messages) + [ctx, cs, y, zs, cum, gain]
    return call(
        functools.partial(finish_kernel, heads, sp_count),
        jax.ShapeDtypeStruct(y.shape, BF16),
        inputs,
        [VMEM] * len(inputs),
        flops=4 * y.size * 256,
        moved=8 * y.size,
        name="finish",
    )


def project_out_kernel(count, *refs):
    pieces, w, *rest = refs[:count], *refs[count:]
    outs, (slot, sem) = rest[:-2], rest[-2:]
    copy = pltpu.make_async_copy(w, slot, sem)
    copy.start()
    copy.wait()
    tp = lax.axis_index("tp")
    total = None
    for q, piece in enumerate(pieces):
        depth = piece.shape[1]
        source = tp ^ q if count > 1 else 0
        rows = slot[pl.ds(pl.multiple_of(source * depth, depth), depth), :] if count > 1 else slot[...]
        part = jnp.dot(piece[...], rows, preferred_element_type=F32)
        total = part if total is None else total + part
    if count == 1:
        outs[0][...] = total.astype(BF16)
        return
    block = outs[0].shape[0]
    for target in range(count):
        value = total[target * block : (target + 1) * block].astype(BF16)
        slot_now = tp ^ target
        for q in range(count):

            @pl.when(slot_now == q)
            def _(q=q, value=value):
                outs[q][...] = value


def project_out(pieces, w):
    count = len(pieces)
    length = pieces[0].shape[0]
    width = w.shape[1]
    if count > 1:
        outs = [jax.ShapeDtypeStruct((length // count, width), BF16)] * count
    else:
        outs = [jax.ShapeDtypeStruct((length, width), BF16)]
    return call(
        functools.partial(project_out_kernel, count),
        outs,
        list(pieces) + [w],
        [VMEM] * count + [HBM],
        [pltpu.VMEM(w.shape, BF16), pltpu.SemaphoreType.DMA(())],
        flops=2 * length * w.size,
        moved=2 * w.size,
        name="project_out",
    )


def residual_kernel(count, *refs):
    updates = refs[:count]
    latent, mods, out = refs[count:]
    tp = lax.axis_index("tp")
    for q, update in enumerate(updates):
        width = update.shape[1]
        cols = pl.ds(pl.multiple_of((tp ^ q) * width, width), width)
        gate = mods[4:5, cols]
        out[:, cols] = (latent[:, cols].astype(F32) + gate * update[...].astype(F32)).astype(BF16)


def residual(updates, latent, mods):
    return call(
        functools.partial(residual_kernel, len(updates)),
        jax.ShapeDtypeStruct(latent.shape, BF16),
        list(updates) + [latent, mods],
        [VMEM] * (len(updates) + 2),
        name="residual",
    )


def per_device(
    latent,
    context,
    cond,
    cond_ctx,
    mod_shift_w,
    mod_scale_w,
    mod_gate_w,
    norm_gain,
    proj_z,
    proj_x,
    proj_b,
    proj_c,
    proj_dt,
    conv_x,
    conv_b,
    conv_c,
    dt_bias,
    decay_log,
    head_gain,
    proj_out,
):
    sp_count, tp_count = lax.axis_size("sp"), lax.axis_size("tp")
    tp = lax.axis_index("tp")
    heads = proj_x.shape[1] // HEAD_DIM
    own, depth = latent.shape
    length = own * tp_count
    ctx_own = context.shape[0]
    ctx_length = ctx_own * sp_count
    fast = direct(tp_count)

    rows = exchange_tp(latent, 0)
    if fast:
        row_places = [
            ((lambda sp, tp, at, q=q: (tp ^ q) * own + at), own, None) for q in range(tp_count)
        ]
    else:
        row_places = [((lambda sp, tp, at: at), length, None)]

    up, down = mod_parts(cond, cond_ctx, latent, mod_shift_w, mod_scale_w, mod_gate_w)
    received = [shift(down if k == sp_count - 1 else up, "sp", k) for k in range(1, sp_count)]
    total = up[:8]
    for part in received:
        total = total + part[:8]
    edge = jnp.where(tp == 0, received[-1][8:], received[0][8:])
    payload = jnp.concatenate([total, edge], axis=0)
    mods, halo = assemble(exchange_tp(payload, 1), tp_count)

    if fast and tp_count >= 4 and ctx_own % 64 == 0:
        context_late, _ = lax.optimization_barrier((context, received[0]))
        part = ctx_own // 4
        mine = lax.dynamic_slice_in_dim(context_late, (tp % 4) * part, part, 0)
        first = [shift(mine, "sp", k) for k in range(1, sp_count)]
        ctx_pieces, ctx_places = [context], [((lambda sp, tp, at: sp * ctx_own + at), ctx_own, None)]
        for k, piece in enumerate(first, 1):
            across = swap(piece, 2)
            for bits, got in ((0, piece), (1, swap(piece, 1)), (2, across), (3, swap(across, 1))):
                ctx_pieces.append(got)
                ctx_places.append(
                    (
                        lambda sp, tp, at, k=k, bits=bits: lax.rem(sp + sp_count - k, sp_count)
                        * ctx_own
                        + lax.rem(tp ^ bits, 4) * part
                        + at,
                        part,
                        None,
                    )
                )
    else:
        ctx_pieces = [lax.all_gather(context, "sp", axis=0, tiled=True)]
        ctx_places = [((lambda sp, tp, at: at), ctx_length, None)]

    common = (
        norm_gain[None],
        padded_row(dt_bias),
        padded_row(decay_log),
        proj_dt,
        conv_x,
        conv_b,
        proj_x,
        proj_b,
    )
    h, xs, bs, cum, cum_t, step_t, *messages = recurrence(
        row_places, rows, length, heads, True, mods, halo, common, sp_count, "latent_states"
    )
    arrived = [shift(message, "sp", k) for k, message in enumerate(messages, 1)]
    cs, y, zs = block_outputs(
        heads, length, sp_count, h, xs, bs, cum, cum_t, step_t, conv_c, proj_c, proj_z
    )
    (ctx_states,) = recurrence(
        ctx_places, ctx_pieces, ctx_length, heads, False, mods, None, common, sp_count, "ctx_states"
    )
    mixed_heads = finish(heads, sp_count, arrived, ctx_states, cs, y, zs, cum, head_gain[None])
    updates = project_out(exchange_tp(mixed_heads, 1), proj_out)
    if fast:
        updates = [updates[0]] + [swap(updates[q], q) for q in range(1, tp_count)]
        return residual(updates, latent, mods)
    update = lax.all_to_all(updates[0], "tp", split_axis=0, concat_axis=1, tiled=True)
    update = lax.optimization_barrier(update).astype(F32)
    return (latent.astype(F32) + mods[4:5] * update).astype(BF16)


def solution(mesh):
    placed = (
        P(("sp", "tp"), None),
        P("sp", None),
        P("sp"),
        P("sp"),
        P("sp", "tp"),
        P("sp", "tp"),
        P("sp", "tp"),
        P(),
        P(None, "tp"),
        P(None, "tp"),
        P(None, "tp"),
        P(None, "tp"),
        P(),
        P(None, "tp"),
        P(None, "tp"),
        P(None, "tp"),
        P("tp"),
        P("tp"),
        P("tp"),
        P(None, "tp"),
    )
    return jax.shard_map(
        per_device, mesh=mesh, in_specs=placed, out_specs=P(("sp", "tp"), None), check_vma=False
    )
```

```python
import functools

import jax
import jax.numpy as jnp
from jax import lax
from jax.experimental import pallas as pl
from jax.experimental.pallas import tpu as pltpu
from jax.sharding import PartitionSpec as P


HEAD_DIM = 64
LANES = 128
EPS = 1e-06
F32 = jnp.float32
BF16 = jnp.bfloat16
VMEM = pl.BlockSpec(memory_space=pltpu.VMEM)
HBM = pl.BlockSpec(memory_space=pltpu.HBM)
MIB = 1024 * 1024
MOST = 63
HINT, HINT_BYTES = 2 * 10**10, 10**8


def silu(u):
    return u * (0.5 * jnp.tanh(0.5 * u) + 0.5)


def size_of(shape):
    count = 1
    for extent in shape.shape:
        count *= extent
    return count * jnp.dtype(shape.dtype).itemsize


def call(kernel, outs, inputs, specs, scratch=(), flops=0, moved=0, spare=4):
    held = sum(min(size_of(x), MIB) for x in inputs)
    held += sum(size_of(x) for x in jax.tree.leaves(outs))
    held += sum(size_of(x) for x in scratch if hasattr(x, "shape") and x.memory_space == pltpu.VMEM)
    return pl.pallas_call(
        kernel,
        out_shape=outs,
        in_specs=specs,
        out_specs=jax.tree.map(lambda _: VMEM, outs),
        scratch_shapes=list(scratch),
        compiler_params=pltpu.CompilerParams(vmem_limit_bytes=min(MOST * MIB, held + spare * MIB)),
        cost_estimate=pl.CostEstimate(flops=flops, bytes_accessed=moved, transcendentals=0),
    )(*inputs)


def shift(array, axis, step):
    count = lax.axis_size(axis)
    return lax.ppermute(array, axis, [(i, (i + step) % count) for i in range(count)])


def swap(array, bits):
    count = lax.axis_size("tp")
    return lax.ppermute(array, "tp", [(i, i ^ bits) for i in range(count)])


def direct(tp_count):
    return tp_count <= 8 and tp_count & (tp_count - 1) == 0 and tp_count > 1


def exchange_tp(array, dim, relay=True):
    count = lax.axis_size("tp")
    if not direct(count):
        return [lax.all_gather(array, "tp", axis=dim, tiled=True)]
    pieces = [array] + [None] * (count - 1)
    for q in range(2, count, 2):
        pieces[q] = swap(array, q)
    for q in range(0, count, 2):
        if relay:
            pieces[q + 1] = swap(pieces[q], 1)
        else:
            pieces[q + 1] = swap(array, q + 1)
    return pieces


def lane_rows(vector):
    return vector.reshape(-1, LANES) if vector.shape[0] % LANES == 0 else vector[None]


def one_row(rows):
    return jnp.concatenate([rows[i : i + 1, :] for i in range(rows.shape[0])], axis=1)


def mod_kernel(cond, cond_ctx, rows, w_shift, w_scale, w_gate, up, down):
    width = w_shift.shape[1]
    acts = [silu(one_row(c[...].astype(F32))) for c in (cond, cond_ctx)]
    both = jnp.concatenate(acts, axis=0).astype(BF16)
    parts = [jnp.dot(both, w[...], preferred_element_type=F32) for w in (w_shift, w_scale, w_gate)]
    mods = jnp.concatenate(parts + [jnp.zeros((2, width), F32)], axis=0)
    pieces = rows.shape[1] // width
    first = rows[0:1, :].astype(F32)
    last = rows[rows.shape[0] - 1 :, :].astype(F32)
    for out, row in ((up, last), (down, first)):
        out[0:8, :] = mods
        for r in range(pieces):
            out[8 + r : 9 + r, :] = row[:, r * width : (r + 1) * width]


def mod_parts(cond, cond_ctx, latent, w_shift, w_scale, w_gate):
    width = w_shift.shape[1]
    shape = jax.ShapeDtypeStruct((8 + latent.shape[1] // width, width), F32)
    return call(
        mod_kernel,
        [shape, shape],
        [lane_rows(cond), lane_rows(cond_ctx), latent, w_shift, w_scale, w_gate],
        [VMEM] * 6,
        flops=12 * w_shift.size,
        moved=6 * w_shift.size,
        spare=MOST,
    )


def assemble_kernel(*refs):
    pieces, mods, halo = refs[:-2], refs[-2], refs[-1]
    tp = lax.axis_index("tp")
    count = len(pieces)
    width = pieces[0].shape[1]
    halo[...] = jnp.zeros_like(halo)
    for q, piece in enumerate(pieces):
        source = tp ^ q
        mods[:, pl.ds(pl.multiple_of(source * width, width), width)] = piece[0:8, :]
        for at, owner in ((0, count - 1), (1, 0)):

            @pl.when(source == owner)
            def _(at=at, piece=piece):
                for r in range(count):
                    halo[at : at + 1, r * width : (r + 1) * width] = piece[8 + r : 9 + r, :]


def assemble(pieces, tp_count):
    if direct(tp_count):
        width = pieces[0].shape[1] * tp_count
        return call(
            assemble_kernel,
            [jax.ShapeDtypeStruct((8, width), F32), jax.ShapeDtypeStruct((8, width), F32)],
            pieces,
            [VMEM] * len(pieces),
            flops=HINT,
            moved=HINT_BYTES,
        )
    (whole,) = pieces
    width = whole.shape[1]
    part = width // tp_count
    before = whole[8:, width - part :].reshape(1, width)
    after = whole[8:, :part].reshape(1, width)
    return whole[:8], jnp.concatenate([before, after, jnp.zeros((6, width), F32)])


def modulate(rows, gain, shift_row):
    wide = rows.astype(F32)
    return wide * lax.rsqrt(jnp.mean(wide * wide, axis=-1, keepdims=True) + EPS) * gain + shift_row


def conv_block(value, length, taps, before, after):
    centre = value[:length]
    row = lax.broadcasted_iota(jnp.int32, centre.shape, 0)
    earlier = jnp.where(row == 0, before, pltpu.roll(centre, 1, 0))
    later = jnp.where(row == length - 1, after, pltpu.roll(centre, length - 1, 0))
    return silu(taps[0:1] * earlier + taps[1:2] * centre + taps[2:3] * later)


def column_blocks(widths):
    blocks = []
    for which, width in enumerate(widths):
        step = min(width, 256)
        blocks += [(which, at, step) for at in range(0, width, step)]
    return blocks


def rounded(value):
    return value.astype(BF16).astype(F32)


def recurrence_kernel(places, length, heads, latent, sp_count, *refs):
    refs = list(refs)
    pieces = [refs.pop(0) for _ in places]
    mods = refs.pop(0)
    halo = refs.pop(0) if latent else None
    gain, bias, decay_log, w_dt, taps_x, taps_b, w_x, w_b = refs[:8]
    refs = refs[8:]
    if latent:
        h, xs, bs, cum_out, cum_t_out, step_t_out = refs[:6]
        messages = refs[6:]
    else:
        states_out, h, xs, bs = refs
    blocks = column_blocks((w_x.shape[1], w_b.shape[1]))
    sp = lax.axis_index("sp")
    tp = lax.axis_index("tp")
    kind = 0 if latent else 1
    shift_row = mods[kind : kind + 1, :]
    gain_row = one_row(gain[...].astype(F32)) * (1.0 + mods[2 + kind : 3 + kind, :])
    for piece, (place, size, group) in zip(pieces, places):
        for at in range(0, piece.shape[0], 16):
            size_now = min(16, piece.shape[0] - at)
            offset = place(sp, tp, at)
            if not isinstance(offset, int):
                offset = pl.multiple_of(offset, 16)
            h[pl.ds(offset, size_now), :] = modulate(
                piece[at : at + size_now, :], gain_row, shift_row
            ).astype(BF16)
    if latent:
        edge = modulate(halo[...], gain_row, shift_row)
        pad = jnp.zeros((h.shape[0] - length - 8, edge.shape[1]), F32)
        h[length:, :] = jnp.concatenate([edge, pad], axis=0).astype(BF16)
    dt = rounded(jnp.dot(h[...], w_dt[...], preferred_element_type=F32))[:length]
    turn = lax.rem(LANES - tp * (2 * heads), LANES)
    dt = pltpu.roll(dt, turn, 1)
    filler = jnp.zeros((1, LANES - bias.shape[1]), F32)
    biased = dt + jnp.concatenate([bias[...], filler], axis=1)
    step = jnp.maximum(biased, 0.0) + jnp.log1p(jnp.exp(-jnp.abs(biased)))
    spent = step * jnp.exp(jnp.concatenate([decay_log[...], filler], axis=1))
    row = lax.broadcasted_iota(jnp.int32, (length, length), 0)
    col = lax.broadcasted_iota(jnp.int32, (length, length), 1)
    lower = jnp.where(row >= col, 1.0, 0.0).astype(F32)
    upper = jnp.where(row <= col, 1.0, 0.0).astype(F32)
    high = lax.Precision.HIGHEST
    prefix = jnp.dot(lower, spent, precision=high, preferred_element_type=F32)
    suffix = jnp.dot(upper, spent, precision=high, preferred_element_type=F32)
    lane = lax.broadcasted_iota(jnp.int32, (length, LANES), 1)
    cum = -jnp.where(lane % 2 == 0, prefix, suffix)
    total = jnp.where(lane[0:1] % 2 == 0, cum[length - 1 : length], cum[0:1])
    weight = jnp.exp(total - cum) * step
    if latent:
        cum_t = cum.T
        cum_out[...] = cum
        cum_t_out[...] = cum_t
        step_t_out[...] = step.T
        extra = messages[0].shape[0] - heads * HEAD_DIM
        rows = extra // 2
        ends = cum_t[0:rows]
        parity = lax.broadcasted_iota(jnp.int32, (rows, 1), 0) % 2
        ends = jnp.where(parity == 0, ends[:, length - 1 : length], ends[:, 0:1])
        decay = jnp.broadcast_to(jnp.exp(ends), (rows, LANES))
        decay_hi = decay.astype(BF16)
        decay_lo = (decay - decay_hi.astype(F32)).astype(BF16)
        for message in messages:
            message[heads * HEAD_DIM : heads * HEAD_DIM + rows, :] = decay_hi
            message[heads * HEAD_DIM + rows :, :] = decay_lo
        has_before = jnp.where(sp > 0, 1.0, 0.0)
        has_after = jnp.where(sp < sp_count - 1, 1.0, 0.0)
    for which, at, width in blocks:
        weights = (w_x, w_b)[which][:, at : at + width]
        value = rounded(jnp.dot(h[...], weights, preferred_element_type=F32))
        taps = (taps_x, taps_b)[which][:, at : at + width].astype(F32)
        if latent:
            before = value[length : length + 1] * has_before
            after = value[length + 1 : length + 2] * has_after
        else:
            before = after = 0.0
        out = conv_block(value, length, taps, before, after)
        (xs, bs)[which][:, at : at + width] = out.astype(BF16)
    state = w_b.shape[1] // heads
    for head in range(heads):
        mine = xs[:, head * HEAD_DIM : (head + 1) * HEAD_DIM].astype(F32)
        pair = jnp.concatenate(
            [mine * weight[:, 2 * head : 2 * head + 1], mine * weight[:, 2 * head + 1 : 2 * head + 2]],
            axis=1,
        ).astype(BF16)
        states = lax.dot_general(
            pair,
            bs[:, head * state : (head + 1) * state],
            (((0,), (0,)), ((), ())),
            preferred_element_type=F32,
        )
        if latent:
            for k, message in enumerate(messages, 1):
                forward = sp + k < sp_count
                chosen = jnp.where(forward, states[:HEAD_DIM], states[HEAD_DIM:])
                message[head * HEAD_DIM : (head + 1) * HEAD_DIM, :] = chosen.astype(BF16)
        else:
            states_out[head * 2 * HEAD_DIM : (head + 1) * 2 * HEAD_DIM, :] = states


def recurrence(places, pieces, length, heads, latent, mods, halo, common, sp_count):
    _, _, _, _, _, _, w_x, w_b = common
    depth = w_x.shape[0]
    state = w_b.shape[1] // heads
    struct = jax.ShapeDtypeStruct
    rows = length + 16 if latent else length
    if latent:
        extra = 2 * max(16, -(-2 * heads // 16) * 16)
        message = struct((heads * HEAD_DIM + extra, state), BF16)
        outs = [
            struct((rows, depth), BF16),
            struct((length, heads * HEAD_DIM), BF16),
            struct((length, heads * state), BF16),
            struct((length, LANES), F32),
            struct((LANES, length), F32),
            struct((LANES, length), F32),
        ] + [message] * (sp_count - 1)
        scratch = []
    else:
        outs = [struct((heads * 2 * HEAD_DIM, state), F32)]
        scratch = [
            pltpu.VMEM((rows, depth), BF16),
            pltpu.VMEM((length, heads * HEAD_DIM), BF16),
            pltpu.VMEM((length, heads * state), BF16),
        ]
    inputs = list(pieces) + [mods] + ([halo] if latent else []) + list(common)
    specs = [VMEM] * len(inputs)
    columns = w_x.shape[1] + w_b.shape[1]
    return call(
        functools.partial(recurrence_kernel, places, length, heads, latent, sp_count),
        outs,
        inputs,
        specs,
        scratch,
        flops=2 * rows * depth * columns,
        moved=2 * depth * columns,
    )


def outputs_kernel(length, heads, sp_count, *refs):
    h, xs, bs, cum, cum_t, step_t, taps_c, w_c, w_z, cs, y, zs = refs
    blocks = column_blocks((w_c.shape[1], w_z.shape[1]))
    sp = lax.axis_index("sp")
    has_before = jnp.where(sp > 0, 1.0, 0.0)
    has_after = jnp.where(sp < sp_count - 1, 1.0, 0.0)
    for which, at, width in blocks:
        weights = (w_c, w_z)[which][:, at : at + width]
        value = rounded(jnp.dot(h[...], weights, preferred_element_type=F32))
        if which == 0:
            before = value[length : length + 1] * has_before
            after = value[length + 1 : length + 2] * has_after
            taps = taps_c[:, at : at + width].astype(F32)
            cs[:, at : at + width] = conv_block(value, length, taps, before, after).astype(BF16)
        else:
            zs[:, at : at + width] = silu(value[:length])
    state = w_c.shape[1] // heads
    row = lax.broadcasted_iota(jnp.int32, (length, length), 0)
    col = lax.broadcasted_iota(jnp.int32, (length, length), 1)
    for head in range(heads):
        f, b = 2 * head, 2 * head + 1
        meet = lax.dot_general(
            cs[:, head * state : (head + 1) * state],
            bs[:, head * state : (head + 1) * state],
            (((1,), (1,)), ((), ())),
            preferred_element_type=F32,
        )
        span = jnp.where(
            row >= col,
            cum[:, f : f + 1] - cum_t[f : f + 1, :],
            cum[:, b : b + 1] - cum_t[b : b + 1, :],
        )
        ahead, behind = step_t[f : f + 1, :], step_t[b : b + 1, :]
        steps = jnp.where(row > col, ahead, jnp.where(row < col, behind, ahead + behind))
        mixed = (meet * jnp.exp(span) * steps).astype(BF16)
        y[:, head * HEAD_DIM : (head + 1) * HEAD_DIM] = jnp.dot(
            mixed, xs[:, head * HEAD_DIM : (head + 1) * HEAD_DIM], preferred_element_type=F32
        )


def block_outputs(heads, length, sp_count, h, xs, bs, cum, cum_t, step_t, taps_c, w_c, w_z):
    struct = jax.ShapeDtypeStruct
    depth = w_c.shape[0]
    columns = w_c.shape[1] + w_z.shape[1]
    return call(
        functools.partial(outputs_kernel, length, heads, sp_count),
        [
            struct((length, w_c.shape[1]), BF16),
            struct((length, w_z.shape[1]), F32),
            struct((length, w_z.shape[1]), F32),
        ],
        [h, xs, bs, cum, cum_t, step_t, taps_c, w_c, w_z],
        [VMEM] * 9,
        flops=2 * h.shape[0] * depth * columns,
        moved=2 * depth * columns,
    )


def finish_kernel(heads, sp_count, *refs):
    messages = refs[: sp_count - 1]
    ctx, cs, y, zs, cum, gain, out = refs[sp_count - 1 :]
    sp = lax.axis_index("sp")
    base = heads * HEAD_DIM
    rows = (messages[0].shape[0] - base) // 2
    decays = [
        m[base : base + rows, :].astype(F32) + m[base + rows :, :].astype(F32) for m in messages
    ]
    one = jnp.ones_like(decays[0])
    zero = jnp.zeros_like(decays[0])
    forward, backward = [None] * (sp_count - 1), [None] * (sp_count - 1)
    run = one
    for k in range(1, sp_count):
        active = k <= sp
        forward[k - 1] = jnp.where(active, run, zero)
        run = jnp.where(active, run * decays[k - 1], run)
    ctx_forward = run
    run = one
    for k in range(sp_count - 1, 0, -1):
        active = k > sp
        backward[k - 1] = jnp.where(active, run, zero)
        run = jnp.where(active, run * decays[k - 1], run)
    ctx_backward = run
    carry = jnp.exp(cum[...])
    gain_row = one_row(gain[...].astype(F32))
    state = cs.shape[1] // heads
    for head in range(heads):
        f, b = 2 * head, 2 * head + 1
        at = head * 2 * HEAD_DIM
        start_f = ctx[at : at + HEAD_DIM, :] * ctx_forward[f : f + 1]
        start_b = ctx[at + HEAD_DIM : at + 2 * HEAD_DIM, :] * ctx_backward[b : b + 1]
        for k in range(sp_count - 1):
            part = messages[k][head * HEAD_DIM : (head + 1) * HEAD_DIM, :].astype(F32)
            start_f = start_f + part * forward[k][f : f + 1]
            start_b = start_b + part * backward[k][b : b + 1]
        start = jnp.concatenate([start_f, start_b], axis=0).astype(BF16)
        carried = lax.dot_general(
            cs[:, head * state : (head + 1) * state],
            start,
            (((1,), (1,)), ((), ())),
            preferred_element_type=F32,
        )
        cols = slice(head * HEAD_DIM, (head + 1) * HEAD_DIM)
        total = (
            y[:, cols]
            + carried[:, :HEAD_DIM] * carry[:, f : f + 1]
            + carried[:, HEAD_DIM:] * carry[:, b : b + 1]
        )
        gated = total * zs[:, cols]
        scale = lax.rsqrt(jnp.mean(gated * gated, axis=-1, keepdims=True) + EPS)
        out[:, cols] = (gated * scale * gain_row[:, cols]).astype(BF16)


def finish(heads, sp_count, messages, ctx, cs, y, zs, cum, gain):
    inputs = list(messages) + [ctx, cs, y, zs, cum, gain]
    return call(
        functools.partial(finish_kernel, heads, sp_count),
        jax.ShapeDtypeStruct(y.shape, BF16),
        inputs,
        [VMEM] * len(inputs),
        flops=4 * y.size * 256,
        moved=8 * y.size,
    )


def project_out_kernel(count, *refs):
    pieces, w, *rest = refs[:count], *refs[count:]
    outs, acc = rest[:-1], rest[-1]
    tp = lax.axis_index("tp")
    total = None
    for q, piece in enumerate(pieces):
        depth = piece.shape[1]
        if count > 1:
            rows = w[pl.ds(pl.multiple_of((tp ^ q) * depth, depth), depth), :]
        else:
            rows = w[...]
        part = jnp.dot(piece[...], rows, preferred_element_type=F32)
        total = part if total is None else total + part
    acc[...] = total
    block = outs[0].shape[0]
    for q, out in enumerate(outs):
        at = pl.multiple_of((tp ^ q) * block, block) if count > 1 else 0
        out[...] = acc[pl.ds(at, block), :].astype(BF16)


def project_out(pieces, w):
    count = len(pieces)
    length = pieces[0].shape[0]
    width = w.shape[1]
    outs = [jax.ShapeDtypeStruct((length // count, width), BF16)] * count
    return call(
        functools.partial(project_out_kernel, count),
        outs,
        list(pieces) + [w],
        [VMEM] * (count + 1),
        [pltpu.VMEM((length, width), F32)],
        flops=2 * length * w.size,
        moved=2 * w.size,
    )


def residual_kernel(count, *refs):
    updates = refs[:count]
    latent, mods, out = refs[count:]
    tp = lax.axis_index("tp")
    for q, update in enumerate(updates):
        width = update.shape[1]
        cols = pl.ds(pl.multiple_of((tp ^ q) * width, width), width)
        gate = mods[4:5, cols]
        out[:, cols] = (latent[:, cols].astype(F32) + gate * update[...].astype(F32)).astype(BF16)


def residual(updates, latent, mods):
    return call(
        functools.partial(residual_kernel, len(updates)),
        jax.ShapeDtypeStruct(latent.shape, BF16),
        list(updates) + [latent, mods],
        [VMEM] * (len(updates) + 2),
    )


def layer(
    latent,
    context,
    cond,
    cond_ctx,
    mod_shift_w,
    mod_scale_w,
    mod_gate_w,
    norm_gain,
    proj_z,
    proj_x,
    proj_b,
    proj_c,
    proj_dt,
    conv_x,
    conv_b,
    conv_c,
    dt_bias,
    decay_log,
    head_gain,
    proj_out,
):
    sp_count, tp_count = lax.axis_size("sp"), lax.axis_size("tp")
    tp = lax.axis_index("tp")
    heads = proj_x.shape[1] // HEAD_DIM
    own, _ = latent.shape
    length = own * tp_count
    ctx_own = context.shape[0]
    ctx_length = ctx_own * sp_count
    fast = direct(tp_count)

    rows = exchange_tp(latent, 0)
    if fast:
        row_places = [
            ((lambda sp, tp, at, q=q: (tp ^ q) * own + at), own, None) for q in range(tp_count)
        ]
    else:
        row_places = [((lambda sp, tp, at: at), length, None)]

    up, down = mod_parts(cond, cond_ctx, latent, mod_shift_w, mod_scale_w, mod_gate_w)
    received = [shift(down if k == sp_count - 1 else up, "sp", k) for k in range(1, sp_count)]
    total = up[:8]
    for part in received:
        total = total + part[:8]
    edge = jnp.where(tp == 0, received[-1][8:], received[0][8:])
    payload = jnp.concatenate([total, edge], axis=0)
    mods, halo = assemble(exchange_tp(payload, 1, False), tp_count)

    if fast and ctx_own % 32 == 0:
        part = ctx_own // 2
        mine = lax.dynamic_slice_in_dim(context, (tp & 1) * part, part, 0)
        halves = [shift(mine, "sp", k) for k in range(1, sp_count)]
    else:
        halves = None

    common = (
        lane_rows(norm_gain),
        dt_bias[None],
        decay_log[None],
        proj_dt,
        conv_x,
        conv_b,
        proj_x,
        proj_b,
    )
    h, xs, bs, cum, cum_t, step_t, *messages = recurrence(
        row_places, rows, length, heads, True, mods, halo, common, sp_count
    )
    arrived = [shift(message, "sp", k) for k, message in enumerate(messages, 1)]
    if halves is not None:
        *halves, h = lax.optimization_barrier((*halves, h))
        ctx_pieces, ctx_places = [context], [((lambda sp, tp, at: sp * ctx_own + at), ctx_own, None)]
        for k, piece in enumerate(halves, 1):
            for bit, got in ((0, piece), (1, swap(piece, 1))):
                ctx_pieces.append(got)
                ctx_places.append(
                    (
                        lambda sp, tp, at, k=k, bit=bit: lax.rem(sp + sp_count - k, sp_count)
                        * ctx_own
                        + ((tp ^ bit) & 1) * part
                        + at,
                        part,
                        None,
                    )
                )
    else:
        ctx_pieces = [lax.all_gather(context, "sp", axis=0, tiled=True)]
        ctx_places = [((lambda sp, tp, at: at), ctx_length, None)]
    cs, y, zs = block_outputs(
        heads, length, sp_count, h, xs, bs, cum, cum_t, step_t, conv_c, proj_c, proj_z
    )
    mods_late, y = lax.optimization_barrier((mods, y))
    (ctx_states,) = recurrence(
        ctx_places, ctx_pieces, ctx_length, heads, False, mods_late, None, common, sp_count
    )
    mixed_heads = finish(heads, sp_count, arrived, ctx_states, cs, y, zs, cum, lane_rows(head_gain))
    updates = project_out(exchange_tp(mixed_heads, 1), proj_out)
    if fast:
        updates = [updates[0]] + [swap(updates[q], q) for q in range(1, tp_count)]
        return residual(updates, latent, mods)
    update = lax.all_to_all(updates[0], "tp", split_axis=0, concat_axis=1, tiled=True)
    update = lax.optimization_barrier(update).astype(F32)
    return (latent.astype(F32) + mods[4:5] * update).astype(BF16)


def solution(mesh):
    placed = (
        P(("sp", "tp"), None),
        P("sp", None),
        P("sp"),
        P("sp"),
        P("sp", "tp"),
        P("sp", "tp"),
        P("sp", "tp"),
        P(),
        P(None, "tp"),
        P(None, "tp"),
        P(None, "tp"),
        P(None, "tp"),
        P(),
        P(None, "tp"),
        P(None, "tp"),
        P(None, "tp"),
        P("tp"),
        P("tp"),
        P("tp"),
        P(None, "tp"),
    )
    return jax.shard_map(
        layer, mesh=mesh, in_specs=placed, out_specs=P(("sp", "tp"), None), check_vma=False
    )
```

```python
import functools

import jax
import jax.numpy as jnp
from jax import lax
from jax.experimental import pallas as pl
from jax.experimental.pallas import tpu as pltpu
from jax.sharding import PartitionSpec as P


HEAD_DIM = 64
LANES = 128
EPS = 1e-06
F32 = jnp.float32
BF16 = jnp.bfloat16
VMEM = pl.BlockSpec(memory_space=pltpu.VMEM)
HBM = pl.BlockSpec(memory_space=pltpu.HBM)
MIB = 1024 * 1024
MOST = 63
HINT, HINT_BYTES = 2 * 10**10, 10**8


def silu(u):
    return u * (0.5 * jnp.tanh(0.5 * u) + 0.5)


def size_of(shape):
    count = 1
    for extent in shape.shape:
        count *= extent
    return count * jnp.dtype(shape.dtype).itemsize


def call(kernel, outs, inputs, specs, scratch=(), flops=0, moved=0, spare=4):
    held = sum(min(size_of(x), MIB) for x in inputs)
    held += sum(size_of(x) for x in jax.tree.leaves(outs))
    held += sum(size_of(x) for x in scratch if hasattr(x, "shape") and x.memory_space == pltpu.VMEM)
    return pl.pallas_call(
        kernel,
        out_shape=outs,
        in_specs=specs,
        out_specs=jax.tree.map(lambda _: VMEM, outs),
        scratch_shapes=list(scratch),
        compiler_params=pltpu.CompilerParams(vmem_limit_bytes=min(MOST * MIB, held + spare * MIB)),
        cost_estimate=pl.CostEstimate(flops=flops, bytes_accessed=moved, transcendentals=0),
    )(*inputs)


def shift(array, axis, step):
    count = lax.axis_size(axis)
    return lax.ppermute(array, axis, [(i, (i + step) % count) for i in range(count)])


def swap(array, bits):
    count = lax.axis_size("tp")
    return lax.ppermute(array, "tp", [(i, i ^ bits) for i in range(count)])


def direct(tp_count):
    return tp_count <= 8 and tp_count & (tp_count - 1) == 0 and tp_count > 1


def exchange_tp(array, dim, relay=True):
    count = lax.axis_size("tp")
    if not direct(count):
        return [lax.all_gather(array, "tp", axis=dim, tiled=True)]
    pieces = [array] + [None] * (count - 1)
    if not relay:
        return [array] + [swap(array, q) for q in range(1, count)]
    for q in range(2, count, 2):
        pieces[q] = swap(array, q)
    for q in range(0, count, 2):
        pieces[q + 1] = swap(pieces[q], 1)
    return pieces


def lane_rows(vector):
    return vector.reshape(-1, LANES) if vector.shape[0] % LANES == 0 else vector[None]


def one_row(rows):
    return jnp.concatenate([rows[i : i + 1, :] for i in range(rows.shape[0])], axis=1)


def mod_kernel(cond, cond_ctx, rows, context, w_shift, w_scale, w_gate, up, down, mine):
    part = mine.shape[0]
    core = lax.axis_index("tp") & 1
    mine[...] = context[pl.ds(pl.multiple_of(core * part, part), part), :]
    width = w_shift.shape[1]
    acts = [silu(one_row(c[...].astype(F32))) for c in (cond, cond_ctx)]
    both = jnp.concatenate(acts, axis=0).astype(BF16)
    parts = [jnp.dot(both, w[...], preferred_element_type=F32) for w in (w_shift, w_scale, w_gate)]
    mods = jnp.concatenate(parts + [jnp.zeros((2, width), F32)], axis=0)
    pieces = rows.shape[1] // width
    first = rows[0:1, :].astype(F32)
    last = rows[rows.shape[0] - 1 :, :].astype(F32)
    for out, row in ((up, last), (down, first)):
        out[0:8, :] = mods
        for r in range(pieces):
            out[8 + r : 9 + r, :] = row[:, r * width : (r + 1) * width]


def mod_parts(cond, cond_ctx, latent, context, w_shift, w_scale, w_gate):
    width = w_shift.shape[1]
    shape = jax.ShapeDtypeStruct((8 + latent.shape[1] // width, width), F32)
    return call(
        mod_kernel,
        [shape, shape, jax.ShapeDtypeStruct((context.shape[0] // 2, context.shape[1]), BF16)],
        [lane_rows(cond), lane_rows(cond_ctx), latent, context, w_shift, w_scale, w_gate],
        [VMEM] * 7,
        flops=12 * w_shift.size,
        moved=6 * w_shift.size,
        spare=MOST,
    )


def assemble_kernel(*refs):
    pieces, mods, halo = refs[:-2], refs[-2], refs[-1]
    tp = lax.axis_index("tp")
    count = len(pieces)
    width = pieces[0].shape[1]
    halo[...] = jnp.zeros_like(halo)
    for q, piece in enumerate(pieces):
        source = tp ^ q
        mods[:, pl.ds(pl.multiple_of(source * width, width), width)] = piece[0:8, :]
        for at, owner in ((0, count - 1), (1, 0)):

            @pl.when(source == owner)
            def _(at=at, piece=piece):
                for r in range(count):
                    halo[at : at + 1, r * width : (r + 1) * width] = piece[8 + r : 9 + r, :]


def assemble(pieces, tp_count):
    if direct(tp_count):
        width = pieces[0].shape[1] * tp_count
        return call(
            assemble_kernel,
            [jax.ShapeDtypeStruct((8, width), F32), jax.ShapeDtypeStruct((8, width), F32)],
            pieces,
            [VMEM] * len(pieces),
            flops=HINT,
            moved=HINT_BYTES,
        )
    (whole,) = pieces
    width = whole.shape[1]
    part = width // tp_count
    before = whole[8:, width - part :].reshape(1, width)
    after = whole[8:, :part].reshape(1, width)
    return whole[:8], jnp.concatenate([before, after, jnp.zeros((6, width), F32)])


def modulate(rows, gain, shift_row):
    wide = rows.astype(F32)
    return wide * lax.rsqrt(jnp.mean(wide * wide, axis=-1, keepdims=True) + EPS) * gain + shift_row


def conv_block(value, length, taps, before, after):
    centre = value[:length]
    row = lax.broadcasted_iota(jnp.int32, centre.shape, 0)
    earlier = jnp.where(row == 0, before, pltpu.roll(centre, 1, 0))
    later = jnp.where(row == length - 1, after, pltpu.roll(centre, length - 1, 0))
    return silu(taps[0:1] * earlier + taps[1:2] * centre + taps[2:3] * later)


def column_blocks(widths):
    blocks = []
    for which, width in enumerate(widths):
        step = min(width, 256)
        blocks += [(which, at, step) for at in range(0, width, step)]
    return blocks


def rounded(value):
    return value.astype(BF16).astype(F32)


def recurrence_kernel(places, length, heads, latent, sp_count, *refs):
    refs = list(refs)
    pieces = [refs.pop(0) for _ in places]
    mods = refs.pop(0)
    halo = refs.pop(0) if latent else None
    gain, bias, decay_log, w_dt, taps_x, taps_b, w_x, w_b = refs[:8]
    refs = refs[8:]
    if latent:
        h, xs, bs, cum_out, cum_t_out, step_t_out = refs[:6]
        messages = refs[6:]
    else:
        states_out, h, xs, bs = refs
    blocks = column_blocks((w_x.shape[1], w_b.shape[1]))
    sp = lax.axis_index("sp")
    tp = lax.axis_index("tp")
    kind = 0 if latent else 1
    shift_row = mods[kind : kind + 1, :]
    gain_row = one_row(gain[...].astype(F32)) * (1.0 + mods[2 + kind : 3 + kind, :])
    for piece, (place, size, group) in zip(pieces, places):
        for at in range(0, piece.shape[0], 16):
            size_now = min(16, piece.shape[0] - at)
            offset = place(sp, tp, at)
            if not isinstance(offset, int):
                offset = pl.multiple_of(offset, 16)
            h[pl.ds(offset, size_now), :] = modulate(
                piece[at : at + size_now, :], gain_row, shift_row
            ).astype(BF16)
    if latent:
        edge = modulate(halo[...], gain_row, shift_row)
        pad = jnp.zeros((h.shape[0] - length - 8, edge.shape[1]), F32)
        h[length:, :] = jnp.concatenate([edge, pad], axis=0).astype(BF16)
    dt = rounded(jnp.dot(h[...], w_dt[...], preferred_element_type=F32))[:length]
    turn = lax.rem(LANES - tp * (2 * heads), LANES)
    dt = pltpu.roll(dt, turn, 1)
    filler = jnp.zeros((1, LANES - bias.shape[1]), F32)
    biased = dt + jnp.concatenate([bias[...], filler], axis=1)
    step = jnp.maximum(biased, 0.0) + jnp.log1p(jnp.exp(-jnp.abs(biased)))
    spent = step * jnp.exp(jnp.concatenate([decay_log[...], filler], axis=1))
    row = lax.broadcasted_iota(jnp.int32, (length, length), 0)
    col = lax.broadcasted_iota(jnp.int32, (length, length), 1)
    lower = jnp.where(row >= col, 1.0, 0.0).astype(BF16)
    upper = jnp.where(row <= col, 1.0, 0.0).astype(BF16)
    prefix = suffix = 0.0
    rest = spent
    for _ in range(3):
        term = rest.astype(BF16)
        rest = rest - term.astype(F32)
        prefix = prefix + jnp.dot(lower, term, preferred_element_type=F32)
        suffix = suffix + jnp.dot(upper, term, preferred_element_type=F32)
    lane = lax.broadcasted_iota(jnp.int32, (length, LANES), 1)
    cum = -jnp.where(lane % 2 == 0, prefix, suffix)
    total = jnp.where(lane[0:1] % 2 == 0, cum[length - 1 : length], cum[0:1])
    weight = jnp.exp(total - cum) * step
    if latent:
        cum_t = cum.T
        cum_out[...] = cum
        cum_t_out[...] = cum_t
        step_t_out[...] = step.T
        extra = messages[0].shape[0] - heads * HEAD_DIM
        rows = extra // 2
        ends = cum_t[0:rows]
        parity = lax.broadcasted_iota(jnp.int32, (rows, 1), 0) % 2
        ends = jnp.where(parity == 0, ends[:, length - 1 : length], ends[:, 0:1])
        decay = jnp.broadcast_to(jnp.exp(ends), (rows, LANES))
        decay_hi = decay.astype(BF16)
        decay_lo = (decay - decay_hi.astype(F32)).astype(BF16)
        for message in messages:
            message[heads * HEAD_DIM : heads * HEAD_DIM + rows, :] = decay_hi
            message[heads * HEAD_DIM + rows :, :] = decay_lo
        has_before = jnp.where(sp > 0, 1.0, 0.0)
        has_after = jnp.where(sp < sp_count - 1, 1.0, 0.0)
    for which, at, width in blocks:
        weights = (w_x, w_b)[which][:, at : at + width]
        value = rounded(jnp.dot(h[...], weights, preferred_element_type=F32))
        taps = (taps_x, taps_b)[which][:, at : at + width].astype(F32)
        if latent:
            before = value[length : length + 1] * has_before
            after = value[length + 1 : length + 2] * has_after
        else:
            before = after = 0.0
        out = conv_block(value, length, taps, before, after)
        (xs, bs)[which][:, at : at + width] = out.astype(BF16)
    state = w_b.shape[1] // heads
    for head in range(heads):
        mine = xs[:, head * HEAD_DIM : (head + 1) * HEAD_DIM].astype(F32)
        pair = jnp.concatenate(
            [mine * weight[:, 2 * head : 2 * head + 1], mine * weight[:, 2 * head + 1 : 2 * head + 2]],
            axis=1,
        ).astype(BF16)
        states = lax.dot_general(
            pair,
            bs[:, head * state : (head + 1) * state],
            (((0,), (0,)), ((), ())),
            preferred_element_type=F32,
        )
        if latent:
            for k, message in enumerate(messages, 1):
                forward = sp + k < sp_count
                chosen = jnp.where(forward, states[:HEAD_DIM], states[HEAD_DIM:])
                message[head * HEAD_DIM : (head + 1) * HEAD_DIM, :] = chosen.astype(BF16)
        else:
            states_out[head * 2 * HEAD_DIM : (head + 1) * 2 * HEAD_DIM, :] = states


def recurrence(places, pieces, length, heads, latent, mods, halo, common, sp_count):
    _, _, _, _, _, _, w_x, w_b = common
    depth = w_x.shape[0]
    state = w_b.shape[1] // heads
    struct = jax.ShapeDtypeStruct
    rows = length + 16 if latent else length
    if latent:
        extra = 2 * max(16, -(-2 * heads // 16) * 16)
        message = struct((heads * HEAD_DIM + extra, state), BF16)
        outs = [
            struct((rows, depth), BF16),
            struct((length, heads * HEAD_DIM), BF16),
            struct((length, heads * state), BF16),
            struct((length, LANES), F32),
            struct((LANES, length), F32),
            struct((LANES, length), F32),
        ] + [message] * (sp_count - 1)
        scratch = []
    else:
        outs = [struct((heads * 2 * HEAD_DIM, state), F32)]
        scratch = [
            pltpu.VMEM((rows, depth), BF16),
            pltpu.VMEM((length, heads * HEAD_DIM), BF16),
            pltpu.VMEM((length, heads * state), BF16),
        ]
    inputs = list(pieces) + [mods] + ([halo] if latent else []) + list(common)
    specs = [VMEM] * len(inputs)
    columns = w_x.shape[1] + w_b.shape[1]
    return call(
        functools.partial(recurrence_kernel, places, length, heads, latent, sp_count),
        outs,
        inputs,
        specs,
        scratch,
        flops=2 * rows * depth * columns,
        moved=2 * depth * columns,
    )


def outputs_kernel(length, heads, sp_count, *refs):
    h, xs, bs, cum, cum_t, step_t, taps_c, w_c, w_z, cs, y, zs = refs
    blocks = column_blocks((w_c.shape[1], w_z.shape[1]))
    sp = lax.axis_index("sp")
    has_before = jnp.where(sp > 0, 1.0, 0.0)
    has_after = jnp.where(sp < sp_count - 1, 1.0, 0.0)
    for which, at, width in blocks:
        weights = (w_c, w_z)[which][:, at : at + width]
        value = rounded(jnp.dot(h[...], weights, preferred_element_type=F32))
        if which == 0:
            before = value[length : length + 1] * has_before
            after = value[length + 1 : length + 2] * has_after
            taps = taps_c[:, at : at + width].astype(F32)
            cs[:, at : at + width] = conv_block(value, length, taps, before, after).astype(BF16)
        else:
            zs[:, at : at + width] = silu(value[:length])
    state = w_c.shape[1] // heads
    row = lax.broadcasted_iota(jnp.int32, (length, length), 0)
    col = lax.broadcasted_iota(jnp.int32, (length, length), 1)
    for head in range(heads):
        f, b = 2 * head, 2 * head + 1
        meet = lax.dot_general(
            cs[:, head * state : (head + 1) * state],
            bs[:, head * state : (head + 1) * state],
            (((1,), (1,)), ((), ())),
            preferred_element_type=F32,
        )
        span = jnp.where(
            row >= col,
            cum[:, f : f + 1] - cum_t[f : f + 1, :],
            cum[:, b : b + 1] - cum_t[b : b + 1, :],
        )
        ahead, behind = step_t[f : f + 1, :], step_t[b : b + 1, :]
        steps = jnp.where(row > col, ahead, jnp.where(row < col, behind, ahead + behind))
        mixed = (meet * jnp.exp(span) * steps).astype(BF16)
        y[:, head * HEAD_DIM : (head + 1) * HEAD_DIM] = jnp.dot(
            mixed, xs[:, head * HEAD_DIM : (head + 1) * HEAD_DIM], preferred_element_type=F32
        )


def block_outputs(heads, length, sp_count, h, xs, bs, cum, cum_t, step_t, taps_c, w_c, w_z):
    struct = jax.ShapeDtypeStruct
    depth = w_c.shape[0]
    columns = w_c.shape[1] + w_z.shape[1]
    return call(
        functools.partial(outputs_kernel, length, heads, sp_count),
        [
            struct((length, w_c.shape[1]), BF16),
            struct((length, w_z.shape[1]), F32),
            struct((length, w_z.shape[1]), F32),
        ],
        [h, xs, bs, cum, cum_t, step_t, taps_c, w_c, w_z],
        [VMEM] * 9,
        flops=2 * h.shape[0] * depth * columns,
        moved=2 * depth * columns,
    )


def finish_kernel(heads, sp_count, *refs):
    messages = refs[: sp_count - 1]
    ctx, cs, y, zs, cum, gain, out = refs[sp_count - 1 :]
    sp = lax.axis_index("sp")
    base = heads * HEAD_DIM
    rows = (messages[0].shape[0] - base) // 2
    decays = [
        m[base : base + rows, :].astype(F32) + m[base + rows :, :].astype(F32) for m in messages
    ]
    one = jnp.ones_like(decays[0])
    zero = jnp.zeros_like(decays[0])
    forward, backward = [None] * (sp_count - 1), [None] * (sp_count - 1)
    run = one
    for k in range(1, sp_count):
        active = k <= sp
        forward[k - 1] = jnp.where(active, run, zero)
        run = jnp.where(active, run * decays[k - 1], run)
    ctx_forward = run
    run = one
    for k in range(sp_count - 1, 0, -1):
        active = k > sp
        backward[k - 1] = jnp.where(active, run, zero)
        run = jnp.where(active, run * decays[k - 1], run)
    ctx_backward = run
    carry = jnp.exp(cum[...])
    gain_row = one_row(gain[...].astype(F32))
    state = cs.shape[1] // heads
    for head in range(heads):
        f, b = 2 * head, 2 * head + 1
        at = head * 2 * HEAD_DIM
        start_f = ctx[at : at + HEAD_DIM, :] * ctx_forward[f : f + 1]
        start_b = ctx[at + HEAD_DIM : at + 2 * HEAD_DIM, :] * ctx_backward[b : b + 1]
        for k in range(sp_count - 1):
            part = messages[k][head * HEAD_DIM : (head + 1) * HEAD_DIM, :].astype(F32)
            start_f = start_f + part * forward[k][f : f + 1]
            start_b = start_b + part * backward[k][b : b + 1]
        start = jnp.concatenate([start_f, start_b], axis=0).astype(BF16)
        carried = lax.dot_general(
            cs[:, head * state : (head + 1) * state],
            start,
            (((1,), (1,)), ((), ())),
            preferred_element_type=F32,
        )
        cols = slice(head * HEAD_DIM, (head + 1) * HEAD_DIM)
        total = (
            y[:, cols]
            + carried[:, :HEAD_DIM] * carry[:, f : f + 1]
            + carried[:, HEAD_DIM:] * carry[:, b : b + 1]
        )
        gated = total * zs[:, cols]
        scale = lax.rsqrt(jnp.mean(gated * gated, axis=-1, keepdims=True) + EPS)
        out[:, cols] = (gated * scale * gain_row[:, cols]).astype(BF16)


def finish(heads, sp_count, messages, ctx, cs, y, zs, cum, gain):
    inputs = list(messages) + [ctx, cs, y, zs, cum, gain]
    return call(
        functools.partial(finish_kernel, heads, sp_count),
        jax.ShapeDtypeStruct(y.shape, BF16),
        inputs,
        [VMEM] * len(inputs),
        flops=4 * y.size * 256,
        moved=8 * y.size,
    )


def partial_out_kernel(first, *refs):
    *pieces, w, acc = refs
    tp = lax.axis_index("tp")
    total = None
    for q, piece in enumerate(pieces, first):
        depth = piece.shape[1]
        rows = w[pl.ds(pl.multiple_of((tp ^ q) * depth, depth), depth), :]
        part = jnp.dot(piece[...], rows, preferred_element_type=F32)
        total = part if total is None else total + part
    acc[...] = total


def project_out_kernel(first, *refs):
    acc, w, *rest = refs
    count = (len(rest) - 1 + first) // 2
    pieces, outs, total_ref = rest[: count - first], rest[count - first : -1], rest[-1]
    tp = lax.axis_index("tp")
    total = acc[...]
    for q, piece in enumerate(pieces, first):
        depth = piece.shape[1]
        rows = w[pl.ds(pl.multiple_of((tp ^ q) * depth, depth), depth), :]
        total = total + jnp.dot(piece[...], rows, preferred_element_type=F32)
    total_ref[...] = total
    block = outs[0].shape[0]
    for q, out in enumerate(outs):
        out[...] = total_ref[pl.ds(pl.multiple_of((tp ^ q) * block, block), block), :].astype(BF16)


def project_out(pieces, w):
    count = len(pieces)
    length = pieces[0].shape[0]
    width = w.shape[1]
    if count == 1:
        return [jnp.dot(pieces[0], w, preferred_element_type=F32).astype(BF16)]
    first = count - 2
    acc = call(
        functools.partial(partial_out_kernel, 0),
        jax.ShapeDtypeStruct((length, width), F32),
        [*pieces[:first], w],
        [VMEM] * (first + 1),
        flops=2 * length * w.size * first // count,
        moved=2 * w.size,
    )
    return call(
        functools.partial(project_out_kernel, first),
        [jax.ShapeDtypeStruct((length // count, width), BF16)] * count,
        [acc, w, *pieces[first:]],
        [VMEM] * (2 + count - first),
        [pltpu.VMEM((length, width), F32)],
        flops=2 * length * w.size * 2 // count,
        moved=2 * w.size,
    )


def residual_kernel(count, *refs):
    updates = refs[:count]
    latent, mods, out = refs[count:]
    tp = lax.axis_index("tp")
    for q, update in enumerate(updates):
        width = update.shape[1]
        cols = pl.ds(pl.multiple_of((tp ^ q) * width, width), width)
        gate = mods[4:5, cols]
        out[:, cols] = (latent[:, cols].astype(F32) + gate * update[...].astype(F32)).astype(BF16)


def residual(updates, latent, mods):
    return call(
        functools.partial(residual_kernel, len(updates)),
        jax.ShapeDtypeStruct(latent.shape, BF16),
        list(updates) + [latent, mods],
        [VMEM] * (len(updates) + 2),
    )


def layer(
    latent,
    context,
    cond,
    cond_ctx,
    mod_shift_w,
    mod_scale_w,
    mod_gate_w,
    norm_gain,
    proj_z,
    proj_x,
    proj_b,
    proj_c,
    proj_dt,
    conv_x,
    conv_b,
    conv_c,
    dt_bias,
    decay_log,
    head_gain,
    proj_out,
):
    sp_count, tp_count = lax.axis_size("sp"), lax.axis_size("tp")
    tp = lax.axis_index("tp")
    heads = proj_x.shape[1] // HEAD_DIM
    own, _ = latent.shape
    length = own * tp_count
    ctx_own = context.shape[0]
    ctx_length = ctx_own * sp_count
    fast = direct(tp_count)

    rows = exchange_tp(latent, 0)
    if fast:
        row_places = [
            ((lambda sp, tp, at, q=q: (tp ^ q) * own + at), own, None) for q in range(tp_count)
        ]
    else:
        row_places = [((lambda sp, tp, at: at), length, None)]

    up, down, mine = mod_parts(cond, cond_ctx, latent, context, mod_shift_w, mod_scale_w, mod_gate_w)
    received = [shift(down if k == sp_count - 1 else up, "sp", k) for k in range(1, sp_count)]
    total = up[:8]
    for part in received:
        total = total + part[:8]
    edge = jnp.where(tp == 0, received[-1][8:], received[0][8:])
    payload = jnp.concatenate([total, edge], axis=0)
    mods, halo = assemble(exchange_tp(payload, 1, False), tp_count)

    if fast and ctx_own % 32 == 0:
        part = ctx_own // 2
        halves = [shift(mine, "sp", k) for k in range(1, sp_count)]
    else:
        halves = None

    common = (
        lane_rows(norm_gain),
        dt_bias[None],
        decay_log[None],
        proj_dt,
        conv_x,
        conv_b,
        proj_x,
        proj_b,
    )
    h, xs, bs, cum, cum_t, step_t, *messages = recurrence(
        row_places, rows, length, heads, True, mods, halo, common, sp_count
    )
    arrived = [shift(message, "sp", k) for k, message in enumerate(messages, 1)]
    if halves is not None:
        ctx_pieces, ctx_places = [context], [((lambda sp, tp, at: sp * ctx_own + at), ctx_own, None)]
        for k, piece in enumerate(halves, 1):
            for bit, got in ((0, piece), (1, swap(piece, 1))):
                ctx_pieces.append(got)
                ctx_places.append(
                    (
                        lambda sp, tp, at, k=k, bit=bit: lax.rem(sp + sp_count - k, sp_count)
                        * ctx_own
                        + ((tp ^ bit) & 1) * part
                        + at,
                        part,
                        None,
                    )
                )
    else:
        ctx_pieces = [lax.all_gather(context, "sp", axis=0, tiled=True)]
        ctx_places = [((lambda sp, tp, at: at), ctx_length, None)]
    cs, y, zs = block_outputs(
        heads, length, sp_count, h, xs, bs, cum, cum_t, step_t, conv_c, proj_c, proj_z
    )
    mods_late, y = lax.optimization_barrier((mods, y))
    (ctx_states,) = recurrence(
        ctx_places, ctx_pieces, ctx_length, heads, False, mods_late, None, common, sp_count
    )
    mixed_heads = finish(heads, sp_count, arrived, ctx_states, cs, y, zs, cum, lane_rows(head_gain))
    updates = project_out(exchange_tp(mixed_heads, 1), proj_out)
    if fast:
        updates = [updates[0]] + [swap(updates[q], q) for q in range(1, tp_count)]
        return residual(updates, latent, mods)
    update = lax.all_to_all(updates[0], "tp", split_axis=0, concat_axis=1, tiled=True)
    update = lax.optimization_barrier(update).astype(F32)
    return (latent.astype(F32) + mods[4:5] * update).astype(BF16)


def solution(mesh):
    placed = (
        P(("sp", "tp"), None),
        P("sp", None),
        P("sp"),
        P("sp"),
        P("sp", "tp"),
        P("sp", "tp"),
        P("sp", "tp"),
        P(),
        P(None, "tp"),
        P(None, "tp"),
        P(None, "tp"),
        P(None, "tp"),
        P(),
        P(None, "tp"),
        P(None, "tp"),
        P(None, "tp"),
        P("tp"),
        P("tp"),
        P("tp"),
        P(None, "tp"),
    )
    return jax.shard_map(
        layer, mesh=mesh, in_specs=placed, out_specs=P(("sp", "tp"), None), check_vma=False
    )
```
